256 devices in a mesh: grp: 2 (over y), sp: 16 (over z), tp: 8 (over x, core).
Axes of the slice: x: 4, y: 2, z: 16, core: 2. Of those that a mesh axis runs over, the one named last changes fastest.
The devices are a block of a 4x16x16 slice.
Arguments:
- tokens: bfloat16 [8192, 8, 2048], P('sp', 'grp'), parts along dimension 1, may hold values from -48 to 48
- query_weight: bfloat16 [2048, 1024], P(None, 'tp'), may hold values from -2 to 2
- key_weight: bfloat16 [2048, 1024], P(None, 'tp'), may hold values from -2 to 2
- value_weight: bfloat16 [2048, 1024], P(None, 'tp'), may hold values from -3 to 3
- mix_gain: float32 [1024], P('tp'), may hold values from 0.1 to 1.9
- out_weight: bfloat16 [1024, 2048], P('tp'), may hold values from -0.1875 to 0.1875
Outputs:
- mixed: bfloat16 [8192, 8, 2048], P(('sp', 'tp'), 'grp'), parts along dimension 1
The draws below stay inside these ranges and needn't reach their ends.
There are 2 independent parts, one for each index of `grp`. The reference program is written for one: setup_inputs(seed, part) draws one part's arguments, and reference() takes and returns one part's arrays. A program takes and returns all parts, laid end to end along the dimension named above; an argument that names none is the same for every part. Nothing has to cross between parts.
All inputs are finite; a program needn't handle non-finite values.
Results may differ from the reference program's by a relative error of at most 0.02.
Values may be sent and summed in bfloat16 or wider, within the bound.
A program may use at most 128 MiB of HBM per device.

```python
import jax
import jax.numpy as jnp
from jax import lax

D = 2048
HEADS = 16
HEAD_DIM = 64
A_W = 1024
BATCH = 4
SEQ = 8192
N_TP = 8


def draw_tokens(key, part):
    normal_part = jax.random.normal(jax.random.fold_in(key, 1), (SEQ, BATCH, D), jnp.float32)
    result = jnp.clip(normal_part, -6.0, 6.0)
    return result.astype(jnp.bfloat16)


def projection_pair(key):
    leading = jnp.clip(jax.random.normal(jax.random.fold_in(key, 11), (D, A_W), jnp.float32), -6.0, 6.0)
    partner = jnp.clip(jax.random.normal(jax.random.fold_in(key, 12), (D, A_W), jnp.float32), -6.0, 6.0)
    return (leading * D ** (-0.5), partner * D ** (-0.5))


def draw_query_weight(key, part):
    leading, partner = projection_pair(key)
    return leading.astype(jnp.bfloat16)


def draw_key_weight(key, part):
    leading, partner = projection_pair(key)
    blended = partner
    return blended.astype(jnp.bfloat16)


def draw_value_weight(key, part):
    normal_part = jnp.clip(jax.random.normal(jax.random.fold_in(key, 21), (D, A_W), jnp.float32), -6.0, 6.0)
    factors = jnp.exp(jax.random.uniform(jax.random.fold_in(key, 22), (HEADS,), jnp.float32, -1.1, 1.1))
    scaled = normal_part * D ** (-0.5) * jnp.repeat(factors, HEAD_DIM)[None, :]
    return scaled.astype(jnp.bfloat16)


def levels(rng, shape, split, smallest, high):
    loudness, own = 1.0, jax.random.fold_in(rng, 6)
    for dim, shards_of in split:
        draws = jnp.exp(jax.random.uniform(jax.random.fold_in(own, dim), (shards_of,), jnp.float32, smallest / len(split), high / len(split)))
        loudness = loudness * jnp.repeat(draws, shape[dim] // shards_of).reshape([-1 if axis == dim else 1 for axis in range(len(shape))])
    return loudness


def bell_draw(rng, extent, spread, most, shards=(), held_as=jnp.bfloat16):
    loudness = levels(rng, extent, shards, -0.22, 0.18) if shards else 1.0
    entries = jax.random.normal(rng, extent, jnp.float32) * spread * loudness
    return jnp.minimum(jnp.maximum(entries, -most), most).astype(held_as)


def setup_inputs(seed: int = 0, part: int = 0) -> dict:
    streams_of = jax.random.split(jax.random.key(seed), 7)
    part_keys = jax.random.split(jax.random.fold_in(streams_of[6], part), 7)
    return {
        "tokens": draw_tokens(jax.random.fold_in(jax.random.fold_in(streams_of[6], part), 71), part),
        "query_weight": draw_query_weight(jax.random.fold_in(streams_of[6], 71), part),
        "key_weight": draw_key_weight(jax.random.fold_in(streams_of[6], 71), part),
        "value_weight": draw_value_weight(jax.random.fold_in(streams_of[6], 71), part),
        "mix_gain": jnp.clip(1.0 + 0.18 * jax.random.normal(streams_of[4], (A_W,), jnp.float32), 0.1, 1.9),
        "out_weight": bell_draw(streams_of[5], (A_W, D), A_W ** -0.5, 0.1875, ((0, 8),)),
    }


PATTERNS = ((128, 1), (512, 4), (2048, 16))
REACH = 128
EPSILON = 1e-06
NEGATIVE = -1e+30

def band_attend(queries, key_rows, value_rows, live_mask):
    lead_shape = queries.shape[:3]
    query_len = queries.shape[3]
    head_size = queries.shape[4]
    block_len = min(REACH, query_len)
    block_count = query_len // block_len
    query_blocks = queries.reshape(lead_shape + (block_count, block_len, head_size))
    if block_count == 1:
        key_ctx = key_rows.reshape(lead_shape + (1, query_len + REACH, head_size))
        value_ctx = value_rows.reshape(lead_shape + (1, query_len + REACH, head_size))
        live_ctx = live_mask.reshape((live_mask.shape[0], 1, query_len + REACH))
    else:
        key_blocks = key_rows.reshape(lead_shape + (block_count + 1, REACH, head_size))
        value_blocks = value_rows.reshape(lead_shape + (block_count + 1, REACH, head_size))
        key_ctx = jnp.concatenate([key_blocks[:, :, :, :-1], key_blocks[:, :, :, 1:]], axis=4)
        value_ctx = jnp.concatenate([value_blocks[:, :, :, :-1], value_blocks[:, :, :, 1:]], axis=4)
        live_blocks = live_mask.reshape((live_mask.shape[0], block_count + 1, REACH))
        live_ctx = jnp.concatenate([live_blocks[:, :-1], live_blocks[:, 1:]], axis=2)
    ctx_width = block_len + REACH
    offset = jnp.arange(ctx_width)[None, :] - jnp.arange(block_len)[:, None]
    in_band = (offset >= 0) & (offset <= REACH)
    valid = in_band[None, None] & live_ctx[:, :, None, :]
    scores = jnp.einsum('gbhnqe,gbhnke->gbhnqk', query_blocks.astype(jnp.float32), key_ctx.astype(jnp.float32)) * head_size ** (-0.5)
    scores = jnp.where(valid[:, None, None], scores, NEGATIVE)
    highest = lax.optimization_barrier(jnp.max(scores, axis=-1, keepdims=True))
    raised = jnp.exp(scores - highest)
    totals = lax.optimization_barrier(jnp.sum(raised, axis=-1, keepdims=True))
    probs = (raised / totals).astype(jnp.bfloat16)
    result = jnp.einsum('gbhnqk,gbhnke->gbhnqe', probs.astype(jnp.float32), value_ctx.astype(jnp.float32)).astype(jnp.bfloat16)
    log_norm = (highest + jnp.log(totals))[..., 0]
    return (result.reshape(lead_shape + (query_len, head_size)), log_norm.reshape(lead_shape + (query_len,)))

def dilated_pattern(queries, context, base, window, stride):
    seq_rows, batch_size, channels = queries.shape
    heads_dev = channels // HEAD_DIM
    query_len = seq_rows // stride
    key_len = query_len + REACH
    query_class = queries.reshape(query_len, stride, batch_size, heads_dev, HEAD_DIM).transpose(1, 2, 3, 0, 4)
    keyval_class = context.reshape(key_len, stride, batch_size, 2 * heads_dev, HEAD_DIM).transpose(1, 2, 3, 0, 4)
    position = jnp.arange(key_len)[None, :] * stride + jnp.arange(stride)[:, None] + base
    result, log_norm = band_attend(query_class, keyval_class[:, :, :heads_dev], keyval_class[:, :, heads_dev:], position >= 0)
    result = result.transpose(3, 0, 1, 2, 4).reshape(seq_rows, batch_size, channels)
    log_norm = log_norm.transpose(3, 0, 1, 2).reshape(seq_rows, batch_size, heads_dev)
    return (result, log_norm)

def reference(tokens, query_weight, key_weight, value_weight, mix_gain, out_weight):
    seq_len, batch_size, width = tokens.shape
    flat = tokens.reshape(seq_len * batch_size, width)

    def project(weight):
        product = jnp.dot(flat, weight, preferred_element_type=jnp.float32).astype(jnp.bfloat16)
        return product.reshape(seq_len, batch_size, weight.shape[1])
    queries = project(query_weight)
    key_values = jnp.concatenate([project(key_weight), project(value_weight)], axis=-1)
    channels = queries.shape[2]
    heads_all = channels // HEAD_DIM

    def one_sequence(pair):
        query_seq, keyval_seq = pair
        query_seq = query_seq[:, None]
        keyval_seq = keyval_seq[:, None]
        results = []
        norms = []
        for window, stride in PATTERNS:
            context = jnp.pad(keyval_seq, ((window, 0), (0, 0), (0, 0)))
            result, log_norm = dilated_pattern(query_seq, context, -window, window, stride)
            results.append(result)
            norms.append(log_norm)
        weights = jax.nn.softmax(jnp.stack(norms, axis=0), axis=0)
        combined = jnp.zeros((seq_len, 1, heads_all, HEAD_DIM), jnp.float32)
        for index in range(len(PATTERNS)):
            combined = combined + weights[index][..., None] * results[index].astype(jnp.float32).reshape(seq_len, 1, heads_all, HEAD_DIM)
        return combined.reshape(seq_len, channels)
    combined = lax.map(one_sequence, (queries.transpose(1, 0, 2), key_values.transpose(1, 0, 2)))
    combined = combined.transpose(1, 0, 2)
    mean_square = lax.optimization_barrier(jnp.sum(combined * combined, axis=-1, keepdims=True)) / channels
    normed = (combined * lax.rsqrt(mean_square + EPSILON) * mix_gain.astype(jnp.float32)).astype(jnp.bfloat16)
    group = channels // N_TP
    total = jnp.zeros((seq_len * batch_size, out_weight.shape[1]), jnp.float32)
    for member in range(N_TP):
        block = normed[..., member * group:(member + 1) * group].reshape(seq_len * batch_size, group)
        partial_out = jnp.dot(block, out_weight[member * group:(member + 1) * group], preferred_element_type=jnp.float32).astype(jnp.bfloat16)
        total = total + partial_out.astype(jnp.float32)
    return total.reshape(seq_len, batch_size, out_weight.shape[1]).astype(jnp.bfloat16)
```

```python
import functools

import jax
import jax.numpy as jnp
from jax import lax
from jax.experimental import pallas as pl
from jax.experimental.pallas import tpu as pltpu
from jax.sharding import PartitionSpec as P

HEAD_DIM = 64
LANES = 128
CLASSES = 4
EPSILON = 1e-06
NEGATIVE = -1e30
BF = jnp.bfloat16
F32 = jnp.float32
MESH_ID = pl.DeviceIdType.MESH


def kernel(
    n_sp, n_tp,
    tokens, wq, wk, wv, gain, wo,
    out,
    tok, wqkv, wall, gall, acc, q_own, kv_own, kv_prev, q_two, q_three,
    o_three, s_three, i_three, t_three, o_two, s_two, i_two, t_two,
    n_loc, s_loc, corner_v, bias0, bias1, biasc, bias2, bias4,
    x_send, x_recv, x_rows,
    tok_sem, w_sem, own_sem,
    q_ss, q_rs, f_ss, f_rs, k_ss, k_rs,
    o3_ss, o3_rs, t3_ss, t3_rs, o2_ss, o2_rs, t2_ss, t2_rs,
    x_ss, x_rs, g_ss, g_rs, w_ss, w_rs, v_ss, v_rs,
):
    batch = tok.shape[2]
    size = tok.shape[1]
    share = size // n_tp
    reach = size // CLASSES
    z = lax.axis_index("sp")
    me = lax.axis_index("tp")

    def along(step):
        return lax.rem(z + step + n_sp, n_sp)

    def peer(step):
        return lax.rem(me + step, n_tp)

    sibling = me + 1 - 2 * lax.rem(me, 2)

    def remote(src, dst, send, recv, axis, where):
        return pltpu.make_async_remote_copy(
            src_ref=src, dst_ref=dst, send_sem=send, recv_sem=recv,
            device_id={axis: where}, device_id_type=MESH_ID,
        )

    def tok_copy(c):
        return pltpu.make_async_copy(tokens.at[:, c], tok.at[c], tok_sem.at[c])

    weights = [
        pltpu.make_async_copy(w, wqkv.at[:, pl.ds(i * LANES, LANES)], w_sem.at[i])
        for i, w in enumerate((wq, wk, wv))
    ]
    for copy in weights:
        copy.start()
    for c in range(CLASSES):
        tok_copy(c).start()
    own_w = pltpu.make_async_copy(wo, wall.at[me], own_sem)
    own_w.start()
    gall[pl.ds(me, 1)] = gain[...][None]

    barrier = pltpu.get_barrier_semaphore()
    for step in (-2, -1, 1, 2):
        pl.semaphore_signal(barrier, inc=1, device_id={"sp": along(step)}, device_id_type=MESH_ID)
    for step in range(1, n_tp):
        pl.semaphore_signal(barrier, inc=1, device_id={"tp": peer(step)}, device_id_type=MESH_ID)

    key = lax.broadcasted_iota(jnp.int32, (size, LANES), 0)
    query = lax.broadcasted_iota(jnp.int32, (size, LANES), 1)

    def log_count(count):
        return jnp.where(
            count == 0, NEGATIVE,
            jnp.where(count == 1, 0.0, jnp.where(count == 2, 0.6931471805599453, 1.0986122886681098)),
        ).astype(F32)

    for diff in range(1 - CLASSES, CLASSES):
        gap = CLASSES * (query - key) + diff
        count = ((gap >= 0) & (gap <= 128)).astype(jnp.int32)
        if diff == 0:
            count = count + ((gap >= 0) & (gap <= 512)).astype(jnp.int32)
            count = count + ((gap >= 0) & (((query - key) & 3) == 0)).astype(jnp.int32)
        bias0[diff + CLASSES - 1] = log_count(count)
    same = (((query - key) & 3) == 0).astype(jnp.int32)
    bias1[...] = log_count((key >= query).astype(jnp.int32) + same)
    bias2[...] = log_count(same)
    bias4[...] = log_count(jnp.where(key >= query, same, 0)) + jnp.where(z >= 1, 0.0, NEGATIVE)
    for c in range(CLASSES):
        gap = CLASSES * size + CLASSES * (query - (size - reach + lax.rem(key, reach))) + c - key // reach
        biasc[c] = log_count((gap <= 128).astype(jnp.int32))

    pl.semaphore_wait(barrier, 4 + n_tp - 1)

    gains = [
        remote(gall.at[me], gall.at[me], g_ss.at[j - 1], g_rs.at[j - 1], "tp", peer(j))
        for j in range(1, n_tp)
    ]
    across = [
        remote(wo, wall.at[me], w_ss.at[j // 2 - 1], w_rs.at[j // 2 - 1], "tp", peer(j))
        for j in range(2, n_tp, 2)
    ]
    for copy in gains + across:
        copy.start()
    beside = [remote(wo, wall.at[me], v_ss.at[0], v_rs.at[0], "tp", sibling)]
    beside[0].start()

    def send_q(c):
        return remote(q_own.at[c], q_two.at[c], q_ss.at[c], q_rs.at[c], "sp", along(-2))

    def pass_q(c):
        return remote(q_two.at[c], q_three.at[c], f_ss.at[c], f_rs.at[c], "sp", along(-1))

    def send_kv(c):
        return remote(kv_own.at[c], kv_prev.at[c], k_ss.at[c], k_rs.at[c], "sp", along(1))

    def send_three(c):
        return (
            remote(o_three.at[c], i_three.at[c], o3_ss.at[c], o3_rs.at[c], "sp", along(1)),
            remote(s_three.at[c], t_three.at[c], t3_ss.at[c], t3_rs.at[c], "sp", along(1)),
        )

    def send_two(c):
        return (
            remote(o_two.at[c], i_two.at[c], o2_ss.at[c], o2_rs.at[c], "sp", along(2)),
            remote(s_two.at[c], t_two.at[c], t2_ss.at[c], t2_rs.at[c], "sp", along(2)),
        )

    for copy in weights:
        copy.wait()

    @pl.loop(0, CLASSES)
    def _(c):
        tok_copy(c).wait()
        rows = tok[c].reshape(size * batch, tok.shape[3])
        product = jnp.dot(rows, wqkv[...], preferred_element_type=F32)
        for i in range(3):
            acc[i] = product[:, i * LANES:(i + 1) * LANES]
        for b in range(batch):
            picked = pl.ds(b, size, stride=batch)
            q_own[c, b] = (acc[0, picked, :] * HEAD_DIM ** (-0.5)).astype(BF)
            kv_own[c, b, 0] = acc[1, picked, :].astype(BF)
            kv_own[c, b, 1] = acc[2, picked, :].T.astype(BF)
        send_q(c).start()
        send_kv(c).start()

    lane = lax.broadcasted_iota(jnp.int32, (1, LANES), 1)
    head0 = jnp.where(lane < HEAD_DIM, 1.0, 0.0).astype(BF)
    head1 = jnp.where(lane < HEAD_DIM, 0.0, 1.0).astype(BF)

    def attend(query_rows, keys, values, bias):
        count = keys.shape[0]
        both = jnp.concatenate([keys * head0, keys * head1], axis=0)
        scores = lax.dot_general(
            both, query_rows, (((1,), (1,)), ((), ())), preferred_element_type=F32
        )
        state = []
        for h in range(2):
            score = scores[h * count:(h + 1) * count] + bias
            top = jnp.max(score, axis=0, keepdims=True)
            raised = jnp.exp(score - top)
            total = jnp.sum(raised, axis=0, keepdims=True)
            part = jnp.dot(
                values[h * HEAD_DIM:(h + 1) * HEAD_DIM], raised.astype(BF),
                preferred_element_type=F32,
            )
            state.append((part, top, total))
        return state

    def merge(one, two):
        merged = []
        for (part_a, top_a, total_a), (part_b, top_b, total_b) in zip(one, two):
            top = jnp.maximum(top_a, top_b)
            by_a, by_b = jnp.exp(top_a - top), jnp.exp(top_b - top)
            merged.append((part_a * by_a + part_b * by_b, top, total_a * by_a + total_b * by_b))
        return merged

    def masked(state, valid):
        return [(part, jnp.where(valid, top, NEGATIVE), total) for part, top, total in state]

    def put(part_ref, stat_ref, c, b, state):
        for h in range(2):
            part, top, total = state[h]
            part_ref[c, b, h * HEAD_DIM:(h + 1) * HEAD_DIM, :] = part.astype(part_ref.dtype)
            stat_ref[c, b, h:h + 1, :] = top
            stat_ref[c, b, 2 + h:3 + h, :] = total

    def get(part_ref, stat_ref, c, b):
        return [
            (
                part_ref[c, b, h * HEAD_DIM:(h + 1) * HEAD_DIM, :].astype(F32),
                stat_ref[c, b, h:h + 1, :],
                stat_ref[c, b, 2 + h:3 + h, :],
            )
            for h in range(2)
        ]

    @pl.loop(0, CLASSES)
    def _(c):
        send_q(c).wait_recv()
        pass_q(c).start()

        @pl.loop(0, batch)
        def _(b):
            keys = jnp.concatenate([kv_own[j, b, 0] for j in range(CLASSES)], axis=0)
            values = jnp.concatenate([kv_own[j, b, 1] for j in range(CLASSES)], axis=1)
            bias = jnp.concatenate([bias0[c - j + CLASSES - 1] for j in range(CLASSES)], axis=0)
            put(n_loc, s_loc, c, b, attend(q_own[c, b], keys, values, bias))

    @pl.loop(0, CLASSES)
    def _(c):
        pass_q(c).wait_recv()
        send_kv(c).wait_recv()
        bias = jnp.concatenate([bias2[...], bias4[...]], axis=0)
        for b in range(batch):
            keys = jnp.concatenate([kv_own[c, b, 0], kv_prev[c, b, 0]], axis=0)
            values = jnp.concatenate([kv_own[c, b, 1], kv_prev[c, b, 1]], axis=1)
            state = masked(attend(q_three[c, b], keys, values, bias), z + 3 < n_sp)
            put(o_three, s_three, c, b, state)
        for copy in send_three(c):
            copy.start()

    @pl.loop(0, CLASSES)
    def _(c):
        for copy in send_three(c):
            copy.wait_recv()
        for b in range(batch):
            state = masked(
                attend(q_two[c, b], kv_own[c, b, 0], kv_own[c, b, 1], bias2[...]), z + 2 < n_sp
            )
            put(o_two, s_two, c, b, merge(state, get(i_three, t_three, c, b)))
        for copy in send_two(c):
            copy.start()

    pick_row = lax.broadcasted_iota(jnp.int32, (LANES, LANES), 0)
    pick_col = lax.broadcasted_iota(jnp.int32, (LANES, LANES), 1)

    @pl.loop(0, batch)
    def _(b):
        gathered = jnp.zeros((LANES, LANES), F32)
        for j in range(CLASSES):
            hot = (pick_row == size - reach + pick_col - j * reach) & (pick_col // reach == j)
            gathered = gathered + jnp.dot(
                kv_prev[j, b, 1], jnp.where(hot, 1.0, 0.0).astype(BF), preferred_element_type=F32
            )
        corner_v[b] = gathered.astype(BF)

    @pl.loop(0, CLASSES)
    def _(c):
        bias = jnp.concatenate([bias1[...], biasc[c]], axis=0)
        for b in range(batch):
            keys = jnp.concatenate(
                [kv_prev[c, b, 0]]
                + [kv_prev[j, b, 0, size - reach:size, :] for j in range(CLASSES)], axis=0
            )
            values = jnp.concatenate([kv_prev[c, b, 1], corner_v[b]], axis=1)
            state = masked(attend(q_own[c, b], keys, values, bias), z >= 1)
            put(n_loc, s_loc, c, b, merge(state, get(n_loc, s_loc, c, b)))

    for j, copy in enumerate(across):
        copy.wait_recv()
        block = wall.at[peer(n_tp - 2 * (j + 1))]
        beside.append(remote(block, block, v_ss.at[j + 1], v_rs.at[j + 1], "tp", sibling))
        beside[-1].start()

    def send_x(c, j):
        to = peer(j)
        rows = pl.ds(pl.multiple_of(to * share, share), share)
        return remote(
            x_send.at[c, :, rows, :], x_recv.at[c, me], x_ss.at[c, j - 1], x_rs.at[c, j - 1],
            "tp", to,
        )

    def finish(c):
        for copy in send_two(c):
            copy.wait_recv()
        for b in range(batch):
            state = merge(get(n_loc, s_loc, c, b), get(i_two, t_two, c, b))
            mixed = jnp.concatenate([part / total for part, _, total in state], axis=0)
            x_send[c, b] = mixed.T.astype(BF)
        for j in range(1, n_tp):
            send_x(c, j).start()
        for b in range(batch):
            x_recv[c, me, b] = x_send[c, b, pl.ds(pl.multiple_of(me * share, share), share), :]

    def project(c):
        for j in range(1, n_tp):
            send_x(c, j).wait_recv()
        squares = jnp.zeros((share * batch, LANES), F32)
        for r in range(n_tp):
            for b in range(batch):
                x_rows[r, pl.ds(b, share, stride=batch), :] = x_recv[c, r, b].astype(F32)
            squares = squares + x_rows[r] * x_rows[r]
        mean = jnp.sum(squares, axis=1, keepdims=True) / (n_tp * LANES)
        scale = lax.rsqrt(mean + EPSILON)
        normed = jnp.concatenate(
            [(x_rows[r] * scale * gall[r]).astype(BF) for r in range(n_tp)], axis=1
        )
        width = out.shape[3]
        step = min(512, width)
        for at in range(0, width, step):
            weight = wall[:, :, at:at + step].reshape(n_tp * LANES, step)
            block = jnp.dot(normed, weight, preferred_element_type=F32).astype(BF)
            out[:, c, :, at:at + step] = block.reshape(share, batch, step)

    finish(0)
    own_w.wait()
    for copy in gains:
        copy.wait_recv()
    for copy in beside:
        copy.wait_recv()

    @pl.loop(1, CLASSES)
    def _(c):
        finish(c)
        project(c - 1)

    project(CLASSES - 1)

    for copy in gains + across + beside:
        copy.wait_send()

    @pl.loop(0, CLASSES)
    def _(c):
        for copy in (send_q(c), pass_q(c), send_kv(c)) + send_three(c) + send_two(c):
            copy.wait_send()
        for j in range(1, n_tp):
            send_x(c, j).wait_send()


def body(n_sp, n_tp, tokens, wq, wk, wv, gain, wo):
    rows, batch, width = tokens.shape
    size = rows // CLASSES
    share = size // n_tp
    tokens = tokens.reshape(size, CLASSES, batch, width)
    any_spec = pl.BlockSpec(memory_space=pl.ANY)
    vmem_spec = pl.BlockSpec(memory_space=pltpu.VMEM)
    blocks = (CLASSES, batch, LANES, LANES)
    stats = (CLASSES, batch, 4, LANES)
    dma = pltpu.SemaphoreType.DMA
    tiles = pltpu.VMEM((LANES, LANES), F32)
    scratch = (
        [
            pltpu.VMEM((CLASSES, size, batch, width), BF),
            pltpu.VMEM((width, 3 * LANES), BF),
            pltpu.VMEM((n_tp, LANES, wo.shape[1]), BF),
            pltpu.VMEM((n_tp, 1, LANES), F32),
            pltpu.VMEM((3, size * batch, LANES), F32),
            pltpu.VMEM(blocks, BF),
            pltpu.VMEM((CLASSES, batch, 2, LANES, LANES), BF),
            pltpu.VMEM((CLASSES, batch, 2, LANES, LANES), BF),
            pltpu.VMEM(blocks, BF),
            pltpu.VMEM(blocks, BF),
        ]
        + [pltpu.VMEM(blocks, BF), pltpu.VMEM(stats, F32)] * 4
        + [
            pltpu.VMEM(blocks, F32),
            pltpu.VMEM(stats, F32),
            pltpu.VMEM((batch, LANES, LANES), BF),
            pltpu.VMEM((2 * CLASSES - 1, LANES, LANES), F32),
            tiles,
            pltpu.VMEM((CLASSES, LANES, LANES), F32),
            tiles,
            tiles,
            pltpu.VMEM(blocks, BF),
            pltpu.VMEM((CLASSES, n_tp, batch, share, LANES), BF),
            pltpu.VMEM((n_tp, share * batch, LANES), F32),
            dma((CLASSES,)),
            dma((3,)),
            dma(()),
        ]
        + [dma((CLASSES,))] * 14
        + [dma((CLASSES, n_tp - 1))] * 2
        + [dma((n_tp - 1,))] * 2
        + [dma((n_tp // 2 - 1,))] * 2
        + [dma((n_tp // 2,))] * 2
    )
    result = pl.pallas_call(
        functools.partial(kernel, n_sp, n_tp),
        out_shape=jax.ShapeDtypeStruct((share, CLASSES, batch, width), BF),
        in_specs=[any_spec] * 4 + [vmem_spec, any_spec],
        out_specs=vmem_spec,
        scratch_shapes=scratch,
        compiler_params=pltpu.CompilerParams(
            collective_id=0, has_side_effects=True, vmem_limit_bytes=60 * 1024 * 1024
        ),
        name="attend_all",
    )(tokens, wq, wk, wv, gain.reshape(1, LANES), wo)
    return result.reshape(share * CLASSES, batch, width)


def solution(mesh):
    in_specs = (
        P("sp", "grp", None),
        P(None, "tp"),
        P(None, "tp"),
        P(None, "tp"),
        P("tp"),
        P("tp", None),
    )
    out_specs = P(("sp", "tp"), "grp", None)
    step = functools.partial(body, mesh.shape["sp"], mesh.shape["tp"])
    return jax.shard_map(step, mesh=mesh, in_specs=in_specs, out_specs=out_specs, check_vma=False)
```

```python
import functools

import jax
import jax.numpy as jnp
from jax import lax
from jax.experimental import pallas as pl
from jax.experimental.pallas import tpu as pltpu
from jax.sharding import PartitionSpec as P

HEAD_DIM = 64
LANES = 128
CLASSES = 4
EPSILON = 1e-06
NEGATIVE = -1e30
BF = jnp.bfloat16
F32 = jnp.float32
MESH_ID = pl.DeviceIdType.MESH


def kernel(
    n_sp, n_tp,
    tokens, wq, wk, wv, gain, wo,
    out,
    tok, wqkv, wall, gall, acc, q_own, kv_own, kv_prev, q_two, q_three,
    o_three, s_three, i_three, t_three, o_two, s_two, i_two, t_two,
    n_loc, s_loc, corner_v, bias0, bias1, biasc, bias2, bias4,
    x_send, x_recv, x_rows,
    tok_sem, w_sem, own_sem,
    q_ss, q_rs, f_ss, f_rs, k_ss, k_rs,
    o3_ss, o3_rs, t3_ss, t3_rs, o2_ss, o2_rs, t2_ss, t2_rs,
    x_ss, x_rs, g_ss, g_rs, w_ss, w_rs, v_ss, v_rs,
):
    batch = tok.shape[2]
    size = tok.shape[1]
    share = size // n_tp
    reach = size // CLASSES
    z = lax.axis_index("sp")
    me = lax.axis_index("tp")

    def along(step):
        return z + step

    def exists(step):
        return (z + step >= 0) if step < 0 else (z + step < n_sp)

    def peer(step):
        return lax.rem(me + step, n_tp)

    sibling = me + 1 - 2 * lax.rem(me, 2)

    def remote(src, dst, send, recv, axis, where):
        return pltpu.make_async_remote_copy(
            src_ref=src, dst_ref=dst, send_sem=send, recv_sem=recv,
            device_id={axis: where}, device_id_type=MESH_ID,
        )

    def tok_copy(c):
        return pltpu.make_async_copy(tokens.at[:, c], tok.at[c], tok_sem.at[c])

    weights = [
        pltpu.make_async_copy(w, wqkv.at[:, pl.ds(i * LANES, LANES)], w_sem.at[i])
        for i, w in enumerate((wq, wk, wv))
    ]
    for copy in weights:
        copy.start()
    for c in range(CLASSES):
        tok_copy(c).start()
    own_w = pltpu.make_async_copy(wo, wall.at[me], own_sem)
    own_w.start()
    gall[pl.ds(me, 1)] = gain[...][None]

    barrier = pltpu.get_barrier_semaphore()
    near = 0
    for step in (-2, -1, 1, 2):
        near = near + exists(step).astype(jnp.int32)

        @pl.when(exists(step))
        def _():
            pl.semaphore_signal(
                barrier, inc=1, device_id={"sp": along(step)}, device_id_type=MESH_ID
            )

    for step in range(1, n_tp):
        pl.semaphore_signal(barrier, inc=1, device_id={"tp": peer(step)}, device_id_type=MESH_ID)

    key = lax.broadcasted_iota(jnp.int32, (size, LANES), 0)
    query = lax.broadcasted_iota(jnp.int32, (size, LANES), 1)

    def log_count(count):
        return jnp.where(
            count == 0, NEGATIVE,
            jnp.where(count == 1, 0.0, jnp.where(count == 2, 0.6931471805599453, 1.0986122886681098)),
        ).astype(F32)

    for diff in range(1 - CLASSES, CLASSES):
        gap = CLASSES * (query - key) + diff
        count = ((gap >= 0) & (gap <= 128)).astype(jnp.int32)
        if diff == 0:
            count = count + ((gap >= 0) & (gap <= 512)).astype(jnp.int32)
            count = count + ((gap >= 0) & (((query - key) & 3) == 0)).astype(jnp.int32)
        bias0[diff + CLASSES - 1] = log_count(count)
    same = (((query - key) & 3) == 0).astype(jnp.int32)
    bias1[...] = log_count((key >= query).astype(jnp.int32) + same)
    bias2[...] = log_count(same)
    bias4[...] = log_count(jnp.where(key >= query, same, 0)) + jnp.where(z >= 1, 0.0, NEGATIVE)

    @pl.when(z < 1)
    def _():
        kv_prev[...] = jnp.zeros_like(kv_prev)
        i_three[...] = jnp.zeros_like(i_three)
        t_three[...] = jnp.full_like(t_three, NEGATIVE)

    @pl.when(z < 2)
    def _():
        i_two[...] = jnp.zeros_like(i_two)
        t_two[...] = jnp.full_like(t_two, NEGATIVE)

    for c in range(CLASSES):
        gap = CLASSES * size + CLASSES * (query - (size - reach + lax.rem(key, reach))) + c - key // reach
        biasc[c] = log_count((gap <= 128).astype(jnp.int32))


    gains = [
        remote(gall.at[me], gall.at[me], g_ss.at[j - 1], g_rs.at[j - 1], "tp", peer(j))
        for j in range(1, n_tp)
    ]
    across = [
        remote(wo, wall.at[me], w_ss.at[j // 2 - 1], w_rs.at[j // 2 - 1], "tp", peer(j))
        for j in range(2, n_tp, 2)
    ]
    beside = [remote(wo, wall.at[me], v_ss.at[0], v_rs.at[0], "tp", sibling)]

    def send_q(c):
        return remote(q_own.at[c], q_two.at[c], q_ss.at[c], q_rs.at[c], "sp", along(-2))

    def pass_q(c):
        return remote(q_two.at[c], q_three.at[c], f_ss.at[c], f_rs.at[c], "sp", along(-1))

    def send_kv(c):
        return remote(kv_own.at[c], kv_prev.at[c], k_ss.at[c], k_rs.at[c], "sp", along(1))

    def send_three(c):
        return (
            remote(o_three.at[c], i_three.at[c], o3_ss.at[c], o3_rs.at[c], "sp", along(1)),
            remote(s_three.at[c], t_three.at[c], t3_ss.at[c], t3_rs.at[c], "sp", along(1)),
        )

    def send_two(c):
        return (
            remote(o_two.at[c], i_two.at[c], o2_ss.at[c], o2_rs.at[c], "sp", along(2)),
            remote(s_two.at[c], t_two.at[c], t2_ss.at[c], t2_rs.at[c], "sp", along(2)),
        )

    for copy in weights:
        copy.wait()

    def project_class(c):
        tok_copy(c).wait()
        rows = tok[c].reshape(size * batch, tok.shape[3])
        product = jnp.dot(rows, wqkv[...], preferred_element_type=F32)
        for i in range(3):
            acc[i] = product[:, i * LANES:(i + 1) * LANES]
        for b in range(batch):
            picked = pl.ds(b, size, stride=batch)
            q_own[c, b] = (acc[0, picked, :] * HEAD_DIM ** (-0.5)).astype(BF)
            kv_own[c, b, 0] = acc[1, picked, :].astype(BF)
            kv_own[c, b, 1] = acc[2, picked, :].T.astype(BF)

    def send_class(c):
        @pl.when(exists(-2))
        def _():
            send_q(c).start()

        @pl.when(exists(1))
        def _():
            send_kv(c).start()

    project_class(0)
    pl.semaphore_wait(barrier, near + n_tp - 1)
    send_class(0)
    for copy in gains + across:
        copy.start()
    beside[0].start()

    @pl.loop(1, CLASSES)
    def _(c):
        project_class(c)
        send_class(c)

    lane = lax.broadcasted_iota(jnp.int32, (1, LANES), 1)
    head0 = jnp.where(lane < HEAD_DIM, 1.0, 0.0).astype(BF)
    head1 = jnp.where(lane < HEAD_DIM, 0.0, 1.0).astype(BF)

    def attend(query_rows, keys, values, bias):
        count = keys.shape[0]
        both = jnp.concatenate([keys * head0, keys * head1], axis=0)
        scores = lax.dot_general(
            both, query_rows, (((1,), (1,)), ((), ())), preferred_element_type=F32
        )
        state = []
        for h in range(2):
            score = scores[h * count:(h + 1) * count] + bias
            top = jnp.max(score, axis=0, keepdims=True)
            raised = jnp.exp(score - top)
            total = jnp.sum(raised, axis=0, keepdims=True)
            part = jnp.dot(
                values[h * HEAD_DIM:(h + 1) * HEAD_DIM], raised.astype(BF),
                preferred_element_type=F32,
            )
            state.append((part, top, total))
        return state

    def merge(one, two):
        merged = []
        for (part_a, top_a, total_a), (part_b, top_b, total_b) in zip(one, two):
            top = jnp.maximum(top_a, top_b)
            by_a, by_b = jnp.exp(top_a - top), jnp.exp(top_b - top)
            merged.append((part_a * by_a + part_b * by_b, top, total_a * by_a + total_b * by_b))
        return merged

    def put(part_ref, stat_ref, c, b, state):
        for h in range(2):
            part, top, total = state[h]
            part_ref[c, b, h * HEAD_DIM:(h + 1) * HEAD_DIM, :] = part.astype(part_ref.dtype)
            stat_ref[c, b, h:h + 1, :] = top
            stat_ref[c, b, 2 + h:3 + h, :] = total

    def get(part_ref, stat_ref, c, b):
        return [
            (
                part_ref[c, b, h * HEAD_DIM:(h + 1) * HEAD_DIM, :].astype(F32),
                stat_ref[c, b, h:h + 1, :],
                stat_ref[c, b, 2 + h:3 + h, :],
            )
            for h in range(2)
        ]

    @pl.loop(0, CLASSES)
    def _(c):
        @pl.when(exists(2))
        def _():
            send_q(c).wait_recv()

            @pl.when(exists(-1))
            def _():
                pass_q(c).start()

        @pl.loop(0, batch)
        def _(b):
            keys = jnp.concatenate([kv_own[j, b, 0] for j in range(CLASSES)], axis=0)
            values = jnp.concatenate([kv_own[j, b, 1] for j in range(CLASSES)], axis=1)
            bias = jnp.concatenate([bias0[c - j + CLASSES - 1] for j in range(CLASSES)], axis=0)
            put(n_loc, s_loc, c, b, attend(q_own[c, b], keys, values, bias))

    @pl.loop(0, CLASSES)
    def _(c):
        @pl.when(exists(-1))
        def _():
            send_kv(c).wait_recv()

        @pl.when(exists(3))
        def _():
            pass_q(c).wait_recv()
            bias = jnp.concatenate([bias2[...], bias4[...]], axis=0)
            for b in range(batch):
                keys = jnp.concatenate([kv_own[c, b, 0], kv_prev[c, b, 0]], axis=0)
                values = jnp.concatenate([kv_own[c, b, 1], kv_prev[c, b, 1]], axis=1)
                put(o_three, s_three, c, b, attend(q_three[c, b], keys, values, bias))
            for copy in send_three(c):
                copy.start()

    @pl.when(exists(2))
    def _():
        @pl.loop(0, CLASSES)
        def _(c):
            @pl.when(exists(-1))
            def _():
                for copy in send_three(c):
                    copy.wait_recv()

            for b in range(batch):
                state = attend(q_two[c, b], kv_own[c, b, 0], kv_own[c, b, 1], bias2[...])
                put(o_two, s_two, c, b, merge(state, get(i_three, t_three, c, b)))
            for copy in send_two(c):
                copy.start()

    pick_row = lax.broadcasted_iota(jnp.int32, (LANES, LANES), 0)
    pick_col = lax.broadcasted_iota(jnp.int32, (LANES, LANES), 1)

    @pl.when(exists(-1))
    def _():
        @pl.loop(0, batch)
        def _(b):
            gathered = jnp.zeros((LANES, LANES), F32)
            for j in range(CLASSES):
                hot = (pick_row == size - reach + pick_col - j * reach) & (pick_col // reach == j)
                gathered = gathered + jnp.dot(
                    kv_prev[j, b, 1], jnp.where(hot, 1.0, 0.0).astype(BF), preferred_element_type=F32
                )
            corner_v[b] = gathered.astype(BF)

        @pl.loop(0, CLASSES)
        def _(c):
            bias = jnp.concatenate([bias1[...], biasc[c]], axis=0)
            for b in range(batch):
                keys = jnp.concatenate(
                    [kv_prev[c, b, 0]]
                    + [kv_prev[j, b, 0, size - reach:size, :] for j in range(CLASSES)], axis=0
                )
                values = jnp.concatenate([kv_prev[c, b, 1], corner_v[b]], axis=1)
                state = attend(q_own[c, b], keys, values, bias)
                put(n_loc, s_loc, c, b, merge(state, get(n_loc, s_loc, c, b)))

    for j, copy in enumerate(across):
        copy.wait_recv()
        block = wall.at[peer(n_tp - 2 * (j + 1))]
        beside.append(remote(block, block, v_ss.at[j + 1], v_rs.at[j + 1], "tp", sibling))
        beside[-1].start()

    def send_x(c, j):
        to = peer(j)
        rows = pl.ds(pl.multiple_of(to * share, share), share)
        return remote(
            x_send.at[c, :, rows, :], x_recv.at[c, me], x_ss.at[c, j - 1], x_rs.at[c, j - 1],
            "tp", to,
        )

    def finish(c):
        @pl.when(exists(-2))
        def _():
            for copy in send_two(c):
                copy.wait_recv()

        for b in range(batch):
            state = merge(get(n_loc, s_loc, c, b), get(i_two, t_two, c, b))
            mixed = jnp.concatenate([part / total for part, _, total in state], axis=0)
            x_send[c, b] = mixed.T.astype(BF)
        for j in range(1, n_tp):
            send_x(c, j).start()
        for b in range(batch):
            x_recv[c, me, b] = x_send[c, b, pl.ds(pl.multiple_of(me * share, share), share), :]

    def project(c):
        for j in range(1, n_tp):
            send_x(c, j).wait_recv()
        squares = jnp.zeros((share * batch, LANES), F32)
        for r in range(n_tp):
            for b in range(batch):
                x_rows[r, pl.ds(b, share, stride=batch), :] = x_recv[c, r, b].astype(F32)
            squares = squares + x_rows[r] * x_rows[r]
        mean = jnp.sum(squares, axis=1, keepdims=True) / (n_tp * LANES)
        scale = lax.rsqrt(mean + EPSILON)
        normed = jnp.concatenate(
            [(x_rows[r] * scale * gall[r]).astype(BF) for r in range(n_tp)], axis=1
        )
        width = out.shape[3]
        step = min(512, width)
        for at in range(0, width, step):
            weight = wall[:, :, at:at + step].reshape(n_tp * LANES, step)
            block = jnp.dot(normed, weight, preferred_element_type=F32).astype(BF)
            out[:, c, :, at:at + step] = block.reshape(share, batch, step)

    finish(0)
    own_w.wait()
    for copy in gains:
        copy.wait_recv()
    for copy in beside:
        copy.wait_recv()

    @pl.loop(1, CLASSES)
    def _(c):
        finish(c)
        project(c - 1)

    project(CLASSES - 1)

    for copy in gains + across + beside:
        copy.wait_send()

    @pl.loop(0, CLASSES)
    def _(c):
        @pl.when(exists(-2))
        def _():
            send_q(c).wait_send()

        @pl.when(exists(1))
        def _():
            send_kv(c).wait_send()

        @pl.when(exists(2))
        def _():
            for copy in send_two(c):
                copy.wait_send()

            @pl.when(exists(-1))
            def _():
                pass_q(c).wait_send()

        @pl.when(exists(3))
        def _():
            for copy in send_three(c):
                copy.wait_send()

        for j in range(1, n_tp):
            send_x(c, j).wait_send()


def body(n_sp, n_tp, tokens, wq, wk, wv, gain, wo):
    rows, batch, width = tokens.shape
    size = rows // CLASSES
    share = size // n_tp
    tokens = tokens.reshape(size, CLASSES, batch, width)
    any_spec = pl.BlockSpec(memory_space=pl.ANY)
    vmem_spec = pl.BlockSpec(memory_space=pltpu.VMEM)
    blocks = (CLASSES, batch, LANES, LANES)
    stats = (CLASSES, batch, 4, LANES)
    dma = pltpu.SemaphoreType.DMA
    tiles = pltpu.VMEM((LANES, LANES), F32)
    scratch = (
        [
            pltpu.VMEM((CLASSES, size, batch, width), BF),
            pltpu.VMEM((width, 3 * LANES), BF),
            pltpu.VMEM((n_tp, LANES, wo.shape[1]), BF),
            pltpu.VMEM((n_tp, 1, LANES), F32),
            pltpu.VMEM((3, size * batch, LANES), F32),
            pltpu.VMEM(blocks, BF),
            pltpu.VMEM((CLASSES, batch, 2, LANES, LANES), BF),
            pltpu.VMEM((CLASSES, batch, 2, LANES, LANES), BF),
            pltpu.VMEM(blocks, BF),
            pltpu.VMEM(blocks, BF),
        ]
        + [pltpu.VMEM(blocks, BF), pltpu.VMEM(stats, F32)] * 4
        + [
            pltpu.VMEM(blocks, F32),
            pltpu.VMEM(stats, F32),
            pltpu.VMEM((batch, LANES, LANES), BF),
            pltpu.VMEM((2 * CLASSES - 1, LANES, LANES), F32),
            tiles,
            pltpu.VMEM((CLASSES, LANES, LANES), F32),
            tiles,
            tiles,
            pltpu.VMEM(blocks, BF),
            pltpu.VMEM((CLASSES, n_tp, batch, share, LANES), BF),
            pltpu.VMEM((n_tp, share * batch, LANES), F32),
            dma((CLASSES,)),
            dma((3,)),
            dma(()),
        ]
        + [dma((CLASSES,))] * 14
        + [dma((CLASSES, n_tp - 1))] * 2
        + [dma((n_tp - 1,))] * 2
        + [dma((n_tp // 2 - 1,))] * 2
        + [dma((n_tp // 2,))] * 2
    )
    result = pl.pallas_call(
        functools.partial(kernel, n_sp, n_tp),
        out_shape=jax.ShapeDtypeStruct((share, CLASSES, batch, width), BF),
        in_specs=[any_spec] * 4 + [vmem_spec, any_spec],
        out_specs=vmem_spec,
        scratch_shapes=scratch,
        compiler_params=pltpu.CompilerParams(
            collective_id=0, has_side_effects=True, vmem_limit_bytes=60 * 1024 * 1024
        ),
        name="attend_all",
    )(tokens, wq, wk, wv, gain.reshape(1, LANES), wo)
    return result.reshape(share * CLASSES, batch, width)


def solution(mesh):
    in_specs = (
        P("sp", "grp", None),
        P(None, "tp"),
        P(None, "tp"),
        P(None, "tp"),
        P("tp"),
        P("tp", None),
    )
    out_specs = P(("sp", "tp"), "grp", None)
    step = functools.partial(body, mesh.shape["sp"], mesh.shape["tp"])
    return jax.shard_map(step, mesh=mesh, in_specs=in_specs, out_specs=out_specs, check_vma=False)
```

```python
import functools

import jax
import jax.numpy as jnp
from jax import lax
from jax.experimental import pallas as pl
from jax.experimental.pallas import tpu as pltpu
from jax.sharding import PartitionSpec as P

HEAD_DIM = 64
LANES = 128
CLASSES = 4
EPSILON = 1e-06
NEGATIVE = -1e30
BF = jnp.bfloat16
F32 = jnp.float32
MESH_ID = pl.DeviceIdType.MESH


def kernel(
    n_sp, n_tp,
    tokens, wq, wk, wv, gain, wo,
    out,
    tok, wqkv, wall, gall, acc, q_own, kv_own, kv_prev, q_two, q_three,
    o_three, s_three, i_three, t_three, o_two, s_two, i_two, t_two,
    n_loc, s_loc, corner_v, bias0, bias1, biasc, bias2, bias4,
    x_send, x_recv, x_rows,
    tok_sem, w_sem, own_sem, in_one, in_two,
    q_ss, q_rs, f_ss, f_rs, k_ss, k_rs,
    o3_ss, o3_rs, t3_ss, t3_rs, o2_ss, o2_rs, t2_ss, t2_rs,
    x_ss, x_rs, g_ss, g_rs, w_ss, w_rs, v_ss, v_rs,
):
    batch = tok.shape[2]
    size = tok.shape[1]
    share = size // n_tp
    reach = size // CLASSES
    z = lax.axis_index("sp")
    me = lax.axis_index("tp")

    def along(step):
        return z + step

    def exists(step):
        return (z + step >= 0) if step < 0 else (z + step < n_sp)

    def peer(step):
        return lax.rem(me + step, n_tp)

    sibling = me + 1 - 2 * lax.rem(me, 2)

    def remote(src, dst, send, recv, axis, where):
        return pltpu.make_async_remote_copy(
            src_ref=src, dst_ref=dst, send_sem=send, recv_sem=recv,
            device_id={axis: where}, device_id_type=MESH_ID,
        )

    def tok_copy(c):
        return pltpu.make_async_copy(tokens.at[:, c], tok.at[c], tok_sem.at[c])

    weights = [
        pltpu.make_async_copy(w, wqkv.at[:, pl.ds(i * LANES, LANES)], w_sem.at[i])
        for i, w in enumerate((wq, wk, wv))
    ]
    for copy in weights:
        copy.start()
    tok_copy(0).start()
    own_w = pltpu.make_async_copy(wo, wall.at[me], own_sem)
    gall[pl.ds(me, 1)] = gain[...][None]

    barrier = pltpu.get_barrier_semaphore()
    near = 0
    for step in (1, 2):
        near = near + exists(step).astype(jnp.int32)

        @pl.when(exists(-step))
        def _():
            pl.semaphore_signal(
                barrier, inc=1, device_id={"sp": along(-step)}, device_id_type=MESH_ID
            )

    for step in range(1, n_tp):
        pl.semaphore_signal(barrier, inc=1, device_id={"tp": peer(step)}, device_id_type=MESH_ID)

    gains = [
        remote(gall.at[me], gall.at[me], g_ss.at[j - 1], g_rs.at[j - 1], "tp", peer(j))
        for j in range(1, n_tp)
    ]
    across = [
        remote(wo, wall.at[me], w_ss.at[j // 2 - 1], w_rs.at[j // 2 - 1], "tp", peer(j))
        for j in range(2, n_tp, 2)
    ]

    def handed(j):
        block = wo if j == 0 else wall.at[peer(n_tp - 2 * j)]
        place = wall.at[me] if j == 0 else block
        return remote(block, place, v_ss.at[j], v_rs.at[j], "tp", sibling)

    beside = [handed(j) for j in range(n_tp // 2)]

    def send_q(c):
        return remote(q_own.at[c], q_two.at[c], q_ss.at[c], q_rs.at[c], "sp", along(-2))

    def pass_q(c):
        return remote(q_two.at[c], q_three.at[c], f_ss.at[c], f_rs.at[c], "sp", along(-1))

    def send_kv(c):
        return remote(kv_own.at[c], kv_prev.at[c], k_ss.at[c], k_rs.at[c], "sp", along(1))

    def send_three(c):
        return (
            remote(o_three.at[c], i_three.at[c], o3_ss.at[c], o3_rs.at[c], "sp", along(1)),
            remote(s_three.at[c], t_three.at[c], t3_ss.at[c], t3_rs.at[c], "sp", along(1)),
        )

    def send_two(c):
        return (
            remote(o_two.at[c], i_two.at[c], o2_ss.at[c], o2_rs.at[c], "sp", along(2)),
            remote(s_two.at[c], t_two.at[c], t2_ss.at[c], t2_rs.at[c], "sp", along(2)),
        )

    for copy in weights:
        copy.wait()

    def project_class(c):
        tok_copy(c).wait()

        @pl.when(c + 1 < CLASSES)
        def _():
            tok_copy(c + 1).start()

        rows = tok[c].reshape(size * batch, tok.shape[3])
        product = jnp.dot(rows, wqkv[...], preferred_element_type=F32)
        for i in range(3):
            acc[i] = product[:, i * LANES:(i + 1) * LANES]
        for b in range(batch):
            picked = pl.ds(b, size, stride=batch)
            q_own[c, b] = (acc[0, picked, :] * HEAD_DIM ** (-0.5)).astype(BF)
            kv_own[c, b, 0] = acc[1, picked, :].astype(BF)
            kv_own[c, b, 1] = acc[2, picked, :].T.astype(BF)

    def start_q(c):
        @pl.when(exists(-2))
        def _():
            send_q(c).start()

    def start_kv(c):
        @pl.when(exists(1))
        def _():
            send_kv(c).start()

    project_class(jnp.int32(0))
    own_w.start()
    pl.semaphore_wait(barrier, near + n_tp - 1)
    start_kv(0)
    for step, sem in ((1, in_one), (2, in_two)):
        @pl.when(exists(step))
        def _():
            pl.semaphore_signal(
                sem, inc=1, device_id={"sp": along(step)}, device_id_type=MESH_ID
            )

    @pl.when(z > 2)
    def _():
        pl.semaphore_wait(in_two, 1)
        start_q(0)

    for copy in gains + across:
        copy.start()
    beside[0].start()

    key = lax.broadcasted_iota(jnp.int32, (size, LANES), 0)
    query = lax.broadcasted_iota(jnp.int32, (size, LANES), 1)

    def log_count(count):
        return jnp.where(
            count == 0, NEGATIVE,
            jnp.where(count == 1, 0.0, jnp.where(count == 2, 0.6931471805599453, 1.0986122886681098)),
        ).astype(F32)

    for diff in range(1 - CLASSES, CLASSES):
        gap = CLASSES * (query - key) + diff
        count = ((gap >= 0) & (gap <= 128)).astype(jnp.int32)
        if diff == 0:
            count = count + ((gap >= 0) & (gap <= 512)).astype(jnp.int32)
            count = count + ((gap >= 0) & (((query - key) & 3) == 0)).astype(jnp.int32)
        bias0[diff + CLASSES - 1] = log_count(count)
    same = (((query - key) & 3) == 0).astype(jnp.int32)
    bias1[...] = log_count((key >= query).astype(jnp.int32) + same)
    bias2[...] = log_count(same)
    bias4[...] = log_count(jnp.where(key >= query, same, 0)) + jnp.where(z >= 1, 0.0, NEGATIVE)

    @pl.when(z < 1)
    def _():
        kv_prev[...] = jnp.zeros_like(kv_prev)
        i_three[...] = jnp.zeros_like(i_three)
        t_three[...] = jnp.full_like(t_three, NEGATIVE)

    @pl.when(z < 2)
    def _():
        i_two[...] = jnp.zeros_like(i_two)
        t_two[...] = jnp.full_like(t_two, NEGATIVE)

    for c in range(CLASSES):
        gap = CLASSES * size + CLASSES * (query - (size - reach + lax.rem(key, reach))) + c - key // reach
        biasc[c] = log_count((gap <= 128).astype(jnp.int32))


    @pl.loop(1, CLASSES)
    def _(c):
        project_class(c)
        start_kv(c)

        @pl.when((c == 1) & (z > 2))
        def _():
            start_q(c)


    lane = lax.broadcasted_iota(jnp.int32, (1, LANES), 1)
    head0 = jnp.where(lane < HEAD_DIM, 1.0, 0.0).astype(BF)
    head1 = jnp.where(lane < HEAD_DIM, 0.0, 1.0).astype(BF)

    def attend(query_rows, keys, values, bias):
        count = keys.shape[0]
        both = jnp.concatenate([keys * head0, keys * head1], axis=0)
        scores = lax.dot_general(
            both, query_rows, (((1,), (1,)), ((), ())), preferred_element_type=F32
        )
        state = []
        for h in range(2):
            score = scores[h * count:(h + 1) * count] + bias
            top = jnp.max(score, axis=0, keepdims=True)
            raised = jnp.exp(score - top)
            total = jnp.sum(raised, axis=0, keepdims=True)
            part = jnp.dot(
                values[h * HEAD_DIM:(h + 1) * HEAD_DIM], raised.astype(BF),
                preferred_element_type=F32,
            )
            state.append((part, top, total))
        return state

    def merge(one, two):
        merged = []
        for (part_a, top_a, total_a), (part_b, top_b, total_b) in zip(one, two):
            top = jnp.maximum(top_a, top_b)
            by_a, by_b = jnp.exp(top_a - top), jnp.exp(top_b - top)
            merged.append((part_a * by_a + part_b * by_b, top, total_a * by_a + total_b * by_b))
        return merged

    def pack(part_ref, stat_ref, c, b, state):
        for h in range(2):
            part, top, total = state[h]
            part_ref[c, b, h * HEAD_DIM:(h + 1) * HEAD_DIM, :] = (part / total).astype(BF)
            stat_ref[c, b, h:h + 1, :] = top + jnp.log(total)

    def unpack(part_ref, stat_ref, c, b):
        return [
            (
                part_ref[c, b, h * HEAD_DIM:(h + 1) * HEAD_DIM, :].astype(F32),
                stat_ref[c, b, h:h + 1, :],
                jnp.ones((1, LANES), F32),
            )
            for h in range(2)
        ]

    def put(part_ref, stat_ref, c, b, state):
        for h in range(2):
            part, top, total = state[h]
            part_ref[c, b, h * HEAD_DIM:(h + 1) * HEAD_DIM, :] = part.astype(part_ref.dtype)
            stat_ref[c, b, h:h + 1, :] = top
            stat_ref[c, b, 2 + h:3 + h, :] = total

    def get(part_ref, stat_ref, c, b):
        return [
            (
                part_ref[c, b, h * HEAD_DIM:(h + 1) * HEAD_DIM, :].astype(F32),
                stat_ref[c, b, h:h + 1, :],
                stat_ref[c, b, 2 + h:3 + h, :],
            )
            for h in range(2)
        ]

    def three_ahead(c):
        @pl.when(exists(-1))
        def _():
            send_kv(c).wait_recv()

        @pl.when(exists(3))
        def _():
            pass_q(c).wait_recv()
            bias = jnp.concatenate([bias2[...], bias4[...]], axis=0)
            for b in range(batch):
                keys = jnp.concatenate([kv_own[c, b, 0], kv_prev[c, b, 0]], axis=0)
                values = jnp.concatenate([kv_own[c, b, 1], kv_prev[c, b, 1]], axis=1)
                pack(o_three, s_three, c, b, attend(q_three[c, b], keys, values, bias))
            for copy in send_three(c):
                copy.start()

    def two_ahead(c):
        @pl.when(exists(2))
        def _():
            @pl.when(exists(-1))
            def _():
                for copy in send_three(c):
                    copy.wait_recv()

            for b in range(batch):
                state = attend(q_two[c, b], kv_own[c, b, 0], kv_own[c, b, 1], bias2[...])
                pack(o_two, s_two, c, b, merge(state, unpack(i_three, t_three, c, b)))
            for copy in send_two(c):
                copy.start()

    def own_shard(c):
        @pl.loop(0, batch)
        def _(b):
            keys = jnp.concatenate([kv_own[j, b, 0] for j in range(CLASSES)], axis=0)
            values = jnp.concatenate([kv_own[j, b, 1] for j in range(CLASSES)], axis=1)
            bias = jnp.concatenate([bias0[c - j + CLASSES - 1] for j in range(CLASSES)], axis=0)
            put(n_loc, s_loc, c, b, attend(q_own[c, b], keys, values, bias))

    def relay(c):
        @pl.when(exists(2))
        def _():
            send_q(c).wait_recv()

            @pl.when(exists(-1))
            def _():
                pass_q(c).start()

    @pl.when(z > 0)
    def _():
        @pl.loop(0, CLASSES)
        def _(c):
            own_shard(c)

            @pl.when(z >= 2)
            def _():
                @pl.when(c == 0)
                def _():
                    pl.semaphore_wait(in_one, 1)

                @pl.when(c < 2)
                def _():
                    relay(c)

                @pl.when((z == 2) & (c == 1))
                def _():
                    pl.semaphore_wait(in_two, 1)
                    for early in range(CLASSES):
                        start_q(early)

                @pl.when(c == 3)
                def _():
                    relay(2)

            @pl.when(z > 2)
            def _():
                @pl.when(c < 2)
                def _():
                    start_q(c + 2)

                @pl.when(c >= 2)
                def _():
                    three_ahead(c - 2)

    @pl.when(z <= 2)
    def _():
        @pl.when(z == 1)
        def _():
            pl.semaphore_wait(in_one, 1)

        @pl.loop(0, CLASSES)
        def _(c):
            @pl.when((z == 1) | ((z == 2) & (c == 2)))
            def _():
                relay(jnp.where(z == 1, c, 3))

            three_ahead(c)

            @pl.when(z == 0)
            def _():
                relay(c)
                two_ahead(c)

        @pl.when(z > 0)
        def _():
            @pl.loop(0, CLASSES)
            def _(c):
                two_ahead(c)

    @pl.when(z > 2)
    def _():
        @pl.loop(0, 2)
        def _(c):
            two_ahead(c)

        relay(3)

        @pl.loop(2, CLASSES)
        def _(c):
            three_ahead(c)

    for j, copy in enumerate(across):
        copy.wait_recv()
        handed(j + 1).start()

    pick_row = lax.broadcasted_iota(jnp.int32, (LANES, LANES), 0)
    pick_col = lax.broadcasted_iota(jnp.int32, (LANES, LANES), 1)

    @pl.when(exists(-1))
    def _():
        @pl.loop(0, batch)
        def _(b):
            gathered = jnp.zeros((LANES, LANES), F32)
            for j in range(CLASSES):
                hot = (pick_row == size - reach + pick_col - j * reach) & (pick_col // reach == j)
                gathered = gathered + jnp.dot(
                    kv_prev[j, b, 1], jnp.where(hot, 1.0, 0.0).astype(BF), preferred_element_type=F32
                )
            corner_v[b] = gathered.astype(BF)

        @pl.loop(0, CLASSES)
        def _(c):
            bias = jnp.concatenate([bias1[...], biasc[c]], axis=0)
            for b in range(batch):
                keys = jnp.concatenate(
                    [kv_prev[c, b, 0]]
                    + [kv_prev[j, b, 0, size - reach:size, :] for j in range(CLASSES)], axis=0
                )
                values = jnp.concatenate([kv_prev[c, b, 1], corner_v[b]], axis=1)
                state = attend(q_own[c, b], keys, values, bias)
                put(n_loc, s_loc, c, b, merge(state, get(n_loc, s_loc, c, b)))

    @pl.when(z > 2)
    def _():
        @pl.loop(2, CLASSES)
        def _(c):
            two_ahead(c)

    @pl.when(z == 0)
    def _():
        @pl.loop(0, CLASSES)
        def _(c):
            own_shard(c)

    def send_x(c, j):
        to = peer(j)
        rows = pl.ds(pl.multiple_of(to * share, share), share)
        return remote(
            x_send.at[c, :, rows, :], x_recv.at[c, me], x_ss.at[c, j - 1], x_rs.at[c, j - 1],
            "tp", to,
        )

    def finish(c):
        @pl.when(exists(-2))
        def _():
            for copy in send_two(c):
                copy.wait_recv()

        for b in range(batch):
            state = merge(get(n_loc, s_loc, c, b), unpack(i_two, t_two, c, b))
            mixed = jnp.concatenate([part / total for part, _, total in state], axis=0)
            x_send[c, b] = mixed.T.astype(BF)
        for j in range(1, n_tp):
            send_x(c, j).start()
        for b in range(batch):
            x_recv[c, me, b] = x_send[c, b, pl.ds(pl.multiple_of(me * share, share), share), :]

    def project(c):
        for j in range(1, n_tp):
            send_x(c, j).wait_recv()
        squares = jnp.zeros((share * batch, LANES), F32)
        for r in range(n_tp):
            for b in range(batch):
                x_rows[r, pl.ds(b, share, stride=batch), :] = x_recv[c, r, b].astype(F32)
            squares = squares + x_rows[r] * x_rows[r]
        mean = jnp.sum(squares, axis=1, keepdims=True) / (n_tp * LANES)
        scale = lax.rsqrt(mean + EPSILON)
        normed = jnp.concatenate(
            [(x_rows[r] * scale * gall[r]).astype(BF) for r in range(n_tp)], axis=1
        )
        width = out.shape[3]
        step = min(512, width)
        for at in range(0, width, step):
            weight = wall[:, :, at:at + step].reshape(n_tp * LANES, step)
            block = jnp.dot(normed, weight, preferred_element_type=F32).astype(BF)
            out[:, c, :, at:at + step] = block.reshape(share, batch, step)

    finish(0)
    own_w.wait()
    for copy in gains:
        copy.wait_recv()
    for copy in beside:
        copy.wait_recv()

    @pl.loop(1, CLASSES)
    def _(c):
        finish(c)
        project(c - 1)

    project(CLASSES - 1)

    for copy in gains + across + beside:
        copy.wait_send()

    @pl.loop(0, CLASSES)
    def _(c):
        @pl.when(exists(-2))
        def _():
            send_q(c).wait_send()

        @pl.when(exists(1))
        def _():
            send_kv(c).wait_send()

        @pl.when(exists(2))
        def _():
            for copy in send_two(c):
                copy.wait_send()

            @pl.when(exists(-1))
            def _():
                pass_q(c).wait_send()

        @pl.when(exists(3))
        def _():
            for copy in send_three(c):
                copy.wait_send()

        for j in range(1, n_tp):
            send_x(c, j).wait_send()


def body(n_sp, n_tp, tokens, wq, wk, wv, gain, wo):
    rows, batch, width = tokens.shape
    size = rows // CLASSES
    share = size // n_tp
    tokens = tokens.reshape(size, CLASSES, batch, width)
    any_spec = pl.BlockSpec(memory_space=pl.ANY)
    vmem_spec = pl.BlockSpec(memory_space=pltpu.VMEM)
    blocks = (CLASSES, batch, LANES, LANES)
    stats = (CLASSES, batch, 2, LANES)
    dma = pltpu.SemaphoreType.DMA
    tiles = pltpu.VMEM((LANES, LANES), F32)
    scratch = (
        [
            pltpu.VMEM((CLASSES, size, batch, width), BF),
            pltpu.VMEM((width, 3 * LANES), BF),
            pltpu.VMEM((n_tp, LANES, wo.shape[1]), BF),
            pltpu.VMEM((n_tp, 1, LANES), F32),
            pltpu.VMEM((3, size * batch, LANES), F32),
            pltpu.VMEM(blocks, BF),
            pltpu.VMEM((CLASSES, batch, 2, LANES, LANES), BF),
            pltpu.VMEM((CLASSES, batch, 2, LANES, LANES), BF),
            pltpu.VMEM(blocks, BF),
            pltpu.VMEM(blocks, BF),
        ]
        + [pltpu.VMEM(blocks, BF), pltpu.VMEM(stats, F32)] * 4
        + [
            pltpu.VMEM(blocks, F32),
            pltpu.VMEM((CLASSES, batch, 4, LANES), F32),
            pltpu.VMEM((batch, LANES, LANES), BF),
            pltpu.VMEM((2 * CLASSES - 1, LANES, LANES), F32),
            tiles,
            pltpu.VMEM((CLASSES, LANES, LANES), F32),
            tiles,
            tiles,
            pltpu.VMEM(blocks, BF),
            pltpu.VMEM((CLASSES, n_tp, batch, share, LANES), BF),
            pltpu.VMEM((n_tp, share * batch, LANES), F32),
            dma((CLASSES,)),
            dma((3,)),
            dma(()),
            pltpu.SemaphoreType.REGULAR,
            pltpu.SemaphoreType.REGULAR,
        ]
        + [dma((CLASSES,))] * 14
        + [dma((CLASSES, n_tp - 1))] * 2
        + [dma((n_tp - 1,))] * 2
        + [dma((n_tp // 2 - 1,))] * 2
        + [dma((n_tp // 2,))] * 2
    )
    result = pl.pallas_call(
        functools.partial(kernel, n_sp, n_tp),
        out_shape=jax.ShapeDtypeStruct((share, CLASSES, batch, width), BF),
        in_specs=[any_spec] * 4 + [vmem_spec, any_spec],
        out_specs=vmem_spec,
        scratch_shapes=scratch,
        compiler_params=pltpu.CompilerParams(
            collective_id=0, has_side_effects=True, vmem_limit_bytes=60 * 1024 * 1024
        ),
        name="attend_all",
    )(tokens, wq, wk, wv, gain.reshape(1, LANES), wo)
    return result.reshape(share * CLASSES, batch, width)


def solution(mesh):
    in_specs = (
        P("sp", "grp", None),
        P(None, "tp"),
        P(None, "tp"),
        P(None, "tp"),
        P("tp"),
        P("tp", None),
    )
    out_specs = P(("sp", "tp"), "grp", None)
    step = functools.partial(body, mesh.shape["sp"], mesh.shape["tp"])
    return jax.shard_map(step, mesh=mesh, in_specs=in_specs, out_specs=out_specs, check_vma=False)
```
